32 devices in a mesh: sp: 8 (over z, x), tp: 4 (over y, core).
Axes of the slice: x: 2, y: 2, z: 4, core: 2. Of those that a mesh axis runs over, the one named last changes fastest.
Arguments:
- residual: bfloat16 [1536, 2048], P(('sp', 'tp')), may hold values from -6 to 6
- query_a: bfloat16 [1536, 1536], P('sp', 'tp'), may hold values from -600 to 600
- query_b: bfloat16 [1536, 2560], P('sp', 'tp'), may hold values from -600 to 600
- latents: bfloat16 [1536, 512], P('sp'), may hold values from -6 to 6
- rope_key: bfloat16 [1536, 32], P('sp'), may hold values from -6 to 6
- key_up_a: bfloat16 [512, 1024], P(None, 'tp'), may hold values from -0.25 to 0.25
- value_up_a: bfloat16 [512, 1024], P(None, 'tp'), may hold values from -0.25 to 0.25
- key_up_b: bfloat16 [512, 2048], P(None, 'tp'), may hold values from -0.25 to 0.25
- value_up_b: bfloat16 [512, 2048], P(None, 'tp'), may hold values from -0.25 to 0.25
- out_proj_a: bfloat16 [1024, 2048], P('tp'), may hold values from -1.5 to 1.5
- out_proj_b: bfloat16 [2048, 2048], P('tp'), may hold values from -1.5 to 1.5
- norm_gain: float32 [2048], replicated, may hold values from 0.1 to 1.9
- routes: int32 [1536, 2], P('sp'), may hold values from 0 to 7, all different within a row; in each aligned block of 192 rows (0 to 191, 192 to 383, ...) at most 72 rows name the same one
- route_weights: float32 [1536, 2], P('sp'), may hold values from 0.2 to 1
- shared_gate: bfloat16 [2048, 2048], P(None, 'tp'), may hold values from -0.125 to 0.125
- shared_up: bfloat16 [2048, 2048], P(None, 'tp'), may hold values from -0.125 to 0.125
- shared_down: bfloat16 [2048, 2048], P('tp'), may hold values from -0.125 to 0.125
- expert_gate: bfloat16 [8, 2048, 2048], P('sp', None, 'tp'), may hold values from -0.125 to 0.125
- expert_up: bfloat16 [8, 2048, 2048], P('sp', None, 'tp'), may hold values from -0.125 to 0.125
- expert_down: bfloat16 [8, 2048, 2048], P('sp', 'tp'), may hold values from -0.125 to 0.125
Outputs:
- layer_out: bfloat16 [1536, 2048], P(('sp', 'tp'))
The draws below stay inside these ranges and needn't reach their ends.
Inputs may be any that keep to these rules, and one draw needn't show every extreme that they name: `routes`: in each aligned block of 192 rows, no expert is named by more than 72 rows, a bound that some block reaches; a row names 2 different experts.
All inputs are finite; a program needn't handle non-finite values.
Results may differ from the reference program's by a relative error of at most 0.022.
The reference program's roundings to bfloat16 on the way count: a program that leaves them out, or rounds other values in their place, can miss the bound.
Values may be sent and summed in bfloat16 or wider, within the bound.
A program may use at most 64 MiB of HBM per device.

```python
import math
import jax
import jax.numpy as jnp
import numpy as np
from jax import lax

D = 2048
HA = 16
HB = 16
DA = 64
VA = 64
DB = 128
VB = 128
ROPE = 32
KV_RANK = 512
EXPERT_FF = 2048
SHARED_FF = 2048
TOPK = 2
TOK_DEV = 192
TOKENS = 1536
EXPERTS = 8
CAP = 72
N_SP = 8
N_TP = 4


def drawn_queries(key, width):
    base = jax.random.normal(key, (TOKENS, width), jnp.float32)
    return jnp.clip(base, -600.0, 600.0).astype(jnp.bfloat16)


def draw_query_a(key, part):
    return drawn_queries(jax.random.fold_in(key, 11), HA * (DA + ROPE))


def draw_query_b(key, part):
    return drawn_queries(jax.random.fold_in(key, 23), HB * (DB + ROPE))


def shard_levels(key, shape, cuts, smallest, top_value):
    def one(position, blocks):
        steps = jax.random.uniform(jax.random.fold_in(jax.random.fold_in(key, 6), position), (blocks,), jnp.float32, smallest / len(cuts), top_value / len(cuts))
        return jnp.repeat(jnp.exp(steps), shape[position] // blocks).reshape((-1,) + (1,) * (len(shape) - position - 1))

    loudness = one(*cuts[0])
    for cut in cuts[1:]:
        loudness = loudness * one(*cut)
    return loudness


def shared_out(stream_key, own, number, rows, amount, top, most, slope):
    ranking = jax.random.permutation(stream_key, amount)
    heavy_load, ordinary = load_shares(amount, rows * top, most, slope, True), load_shares(amount, rows * top, most, slope, False)
    places = jnp.arange(amount)

    def named(sizes, offset_by):
        used = int((sizes > 0).sum())
        fixed = max(1, used // 4)
        passed = fixed + (places - fixed + offset_by * (used - fixed)) % max(1, amount - fixed)
        return jnp.zeros((amount,), jnp.int32).at[ranking[jnp.where(places < fixed, places, passed)]].set(jnp.asarray(sizes, jnp.int32))

    sizes = jnp.where(number % 4 == 0, named(heavy_load, number // 4), named(ordinary, number - number // 4 - 1))
    mixed = jax.random.permutation(jax.random.fold_in(own, 3), amount)
    giver, sink = mixed[0:amount // 2 * 2:2], mixed[1:amount // 2 * 2:2]
    slack = jnp.minimum(sizes[giver] - 1, most - sizes[sink]) // 2
    slack = jnp.where((giver == ranking[0]) | (sink == ranking[0]) | (sizes[sink] == 0), 0, jnp.maximum(slack, 0))
    passed = jax.random.randint(jax.random.fold_in(own, 4), (amount // 2,), 0, 1 << 20) % (slack + 1)
    sizes = sizes.at[giver].add(-passed).at[sink].add(passed)
    labels = jnp.searchsorted(jnp.cumsum(sizes), jnp.arange(rows * top), side="right").astype(jnp.int32)
    listing = labels.reshape(top, rows).T
    listing = listing[jax.random.permutation(jax.random.fold_in(own, 1), rows)]
    offset_by = jax.random.randint(jax.random.fold_in(own, 2), (rows, 1), 0, top)
    return jnp.take_along_axis(listing, (jnp.arange(top)[None, :] + offset_by) % top, axis=1)


def load_shares(number_of, total, limit, skew, full):
    loads = [(1 << 20) // math.isqrt(standing ** skew) + 1 for standing in range(1, number_of + 1)]
    largest = limit if full else min(limit, max(-(-total // number_of), total * loads[0] // sum(loads)))
    least = 1 if total - largest >= number_of - 1 else 0
    given, surplus = [largest] + [least] * (number_of - 1), total - largest - least * (number_of - 1)
    while surplus > 0:
        candidates = [i for i in range(1, number_of) if given[i] < largest] or [i for i in range(1, number_of) if given[i] < limit]
        whole, remaining = sum([loads[i] for i in candidates]), surplus
        for i in candidates:
            addition = min(limit - given[i], max(1, remaining * loads[i] // whole), surplus)
            given[i] = given[i] + addition
            surplus = surplus - addition
    return np.array(given)


def bell_draw(stream_key, extent, spread, most, shards=(), kind=jnp.bfloat16):
    gain = shard_levels(stream_key, extent, shards, -0.22, 0.18) if shards else 1.0
    values = jax.random.normal(stream_key, extent, jnp.float32) * spread * gain
    return jnp.minimum(jnp.maximum(values, -most), most).astype(kind)


def setup_inputs(seed: int = 0) -> dict:
    arg_keys = jax.random.split(jax.random.key(seed), 21)
    residual = bell_draw(arg_keys[0], (TOKENS, D), 1.0, 6.0, ((0, 32),))
    query_a = draw_query_a(jax.random.fold_in(arg_keys[20], 71), 0)
    query_b = draw_query_b(jax.random.fold_in(arg_keys[20], 71), 0)
    latents = bell_draw(arg_keys[3], (TOKENS, KV_RANK), 1.0, 6.0, ((0, 8),))
    rope_key = bell_draw(arg_keys[4], (TOKENS, ROPE), 1.0, 6.0, ((0, 8),))
    key_up_a = bell_draw(arg_keys[5], (KV_RANK, HA * DA), KV_RANK ** -0.5, 0.25, ((1, 4),))
    value_up_a = bell_draw(arg_keys[6], (KV_RANK, HA * VA), KV_RANK ** -0.5, 0.25, ((1, 4),))
    key_up_b = bell_draw(arg_keys[7], (KV_RANK, HB * DB), KV_RANK ** -0.5, 0.25, ((1, 4),))
    value_up_b = bell_draw(arg_keys[8], (KV_RANK, HB * VB), KV_RANK ** -0.5, 0.25, ((1, 4),))
    out_proj_a = bell_draw(arg_keys[9], (HA * VA, D), HA ** -0.5, 1.5, ((0, 4),))
    out_proj_b = bell_draw(arg_keys[10], (HB * VB, D), HA ** -0.5, 1.5, ((0, 4),))
    norm_gain = jnp.clip(1.0 + 0.18 * jax.random.normal(arg_keys[11], (D,), jnp.float32), 0.1, 1.9)
    routes_keys = jax.random.split(jax.random.fold_in(arg_keys[12], 1), TOKENS // TOK_DEV)
    routes_turns = jax.random.permutation(jax.random.fold_in(arg_keys[12], 3), TOKENS // TOK_DEV)
    routes = jax.vmap(lambda own, number: shared_out(jax.random.fold_in(arg_keys[12], 2), own, number, TOK_DEV, EXPERTS, TOPK, CAP, 1))(routes_keys, routes_turns).reshape((TOKENS, TOPK))
    route_weights = jnp.clip(0.2 + 0.8 * jax.random.uniform(arg_keys[13], (TOKENS, TOPK), jnp.float32) ** shard_levels(arg_keys[13], (TOKENS, TOPK), ((0, 8),), -0.2, 0.2), 0.2, 1.0)
    shared_gate = bell_draw(arg_keys[14], (D, SHARED_FF), D ** -0.5, 0.125, ((1, 4),))
    shared_up = bell_draw(arg_keys[15], (D, SHARED_FF), D ** -0.5, 0.125, ((1, 4),))
    shared_down = bell_draw(arg_keys[16], (SHARED_FF, D), SHARED_FF ** -0.5, 0.125, ((0, 4),))
    expert_gate = bell_draw(arg_keys[17], (EXPERTS, D, EXPERT_FF), D ** -0.5, 0.125, ((0, 8), (2, 4)))
    expert_up = bell_draw(arg_keys[18], (EXPERTS, D, EXPERT_FF), D ** -0.5, 0.125, ((0, 8), (2, 4)))
    expert_down = bell_draw(arg_keys[19], (EXPERTS, EXPERT_FF, D), EXPERT_FF ** -0.5, 0.125, ((0, 8), (1, 4)))
    return dict(residual=residual, query_a=query_a, query_b=query_b, latents=latents, rope_key=rope_key, key_up_a=key_up_a, value_up_a=value_up_a, key_up_b=key_up_b, value_up_b=value_up_b, out_proj_a=out_proj_a, out_proj_b=out_proj_b, norm_gain=norm_gain, routes=routes, route_weights=route_weights, shared_gate=shared_gate, shared_up=shared_up, shared_down=shared_down, expert_gate=expert_gate, expert_up=expert_up, expert_down=expert_down)


theta_base = 10000.0
norm_eps = 1e-06

def round_trip(values):
    return lax.optimization_barrier(values.astype(jnp.bfloat16)).astype(jnp.float32)

def tables(positions):
    half = ROPE // 2
    freqs = theta_base ** (-(2.0 * jnp.arange(half, dtype=jnp.float32)) / ROPE)
    angles = positions.astype(jnp.float32)[:, None] * freqs[None, :]
    return (jnp.cos(angles), jnp.sin(angles))

def rotate(values, cosine, sine):
    half = values.shape[-1] // 2
    first = values[..., :half].astype(jnp.float32)
    second = values[..., half:].astype(jnp.float32)
    turned = jnp.concatenate([first * cosine - second * sine, first * sine + second * cosine], axis=-1)
    return turned.astype(jnp.bfloat16)

def attend(queries, keys, values, rot_key, heads, nope, vsize, cosine, sine):
    length = queries.shape[0]
    block = math.gcd(length, 512)
    shaped = queries.reshape(length, heads, nope + ROPE)
    q_nope = shaped[..., :nope]
    q_rope = rotate(shaped[..., nope:], cosine[:, None, :], sine[:, None, :])
    key_all = keys.reshape(length, heads, nope).astype(jnp.float32)
    value_all = values.reshape(length, heads, vsize).astype(jnp.float32)
    rot_all = rot_key.astype(jnp.float32)
    scale = (nope + ROPE) ** (-0.5)
    key_pos = jnp.arange(length, dtype=jnp.int32)

    def one_block(index):
        start = (index * block).astype(jnp.int32)
        q_first = lax.dynamic_slice_in_dim(q_nope, start, block, 0).astype(jnp.float32)
        q_second = lax.dynamic_slice_in_dim(q_rope, start, block, 0).astype(jnp.float32)
        scores = jnp.einsum('qhd,khd->hqk', q_first, key_all) + jnp.einsum('qhr,kr->hqk', q_second, rot_all)
        scores = scores * scale
        query_pos = start + jnp.arange(block, dtype=jnp.int32)
        mask = key_pos[None, :] <= query_pos[:, None]
        top = lax.optimization_barrier(jnp.max(jnp.where(mask[None], scores, -jnp.inf), axis=-1, keepdims=True))
        expo = jnp.where(mask[None], jnp.exp(scores - top), 0.0)
        total = lax.optimization_barrier(jnp.sum(expo, axis=-1))
        weighted = jnp.einsum('hqk,khv->hqv', round_trip(expo), value_all)
        result = (weighted / total[..., None]).astype(jnp.bfloat16)
        return jnp.transpose(result, (1, 0, 2)).reshape(block, heads * vsize)
    blocks = lax.map(one_block, jnp.arange(length // block, dtype=jnp.int32))
    return blocks.reshape(length, heads * vsize)

def reference(residual, query_a, query_b, latents, rope_key, key_up_a, value_up_a, key_up_b, value_up_b, out_proj_a, out_proj_b, norm_gain, routes, route_weights, shared_gate, shared_up, shared_down, expert_gate, expert_up, expert_down):
    positions = jnp.arange(TOKENS, dtype=jnp.int32)
    cosine, sine = tables(positions)
    rot_key = rotate(rope_key, cosine, sine)
    keys_a = jnp.dot(latents, key_up_a, preferred_element_type=jnp.float32).astype(jnp.bfloat16)
    values_a = jnp.dot(latents, value_up_a, preferred_element_type=jnp.float32).astype(jnp.bfloat16)
    keys_b = jnp.dot(latents, key_up_b, preferred_element_type=jnp.float32).astype(jnp.bfloat16)
    values_b = jnp.dot(latents, value_up_b, preferred_element_type=jnp.float32).astype(jnp.bfloat16)
    heads_a = attend(query_a, keys_a, values_a, rot_key, HA, DA, VA, cosine, sine)
    heads_b = attend(query_b, keys_b, values_b, rot_key, HB, DB, VB, cosine, sine)
    width_a = HA * VA // N_TP
    width_b = HB * VB // N_TP

    def head_block(total, index):
        part = jnp.dot(lax.dynamic_slice_in_dim(heads_a, index * width_a, width_a, 1), lax.dynamic_slice_in_dim(out_proj_a, index * width_a, width_a, 0), preferred_element_type=jnp.float32)
        part = part + jnp.dot(lax.dynamic_slice_in_dim(heads_b, index * width_b, width_b, 1), lax.dynamic_slice_in_dim(out_proj_b, index * width_b, width_b, 0), preferred_element_type=jnp.float32)
        return (total + round_trip(part), None)
    mixed, _ = lax.scan(head_block, jnp.zeros((TOKENS, D), jnp.float32), jnp.arange(N_TP, dtype=jnp.int32))
    hidden_state = (residual.astype(jnp.float32) + mixed).astype(jnp.bfloat16)
    wide = hidden_state.astype(jnp.float32)
    normed = (wide * lax.rsqrt(lax.optimization_barrier(jnp.mean(wide * wide, axis=-1, keepdims=True)) + norm_eps) * norm_gain.astype(jnp.float32)).astype(jnp.bfloat16)
    flat = routes.reshape(-1).astype(jnp.int32)
    owners = jnp.arange(TOKENS * TOPK, dtype=jnp.int32) // TOPK
    weights_flat = route_weights.reshape(-1).astype(jnp.float32)
    bound = N_SP * CAP

    def select(expert):
        order = jnp.argsort(jnp.where(flat == expert, 0, 1).astype(jnp.int32), stable=True)[:bound].astype(jnp.int32)
        chosen = jnp.where(flat[order] == expert, weights_flat[order], 0.0)
        return (owners[order], chosen)
    rows_of, weight_of = lax.map(select, jnp.arange(EXPERTS, dtype=jnp.int32))
    expert_width = EXPERT_FF // N_TP
    shared_width = SHARED_FF // N_TP

    def width_block(total, index):
        s_gate = lax.dynamic_slice_in_dim(shared_gate, index * shared_width, shared_width, 1)
        s_up = lax.dynamic_slice_in_dim(shared_up, index * shared_width, shared_width, 1)
        s_down = lax.dynamic_slice_in_dim(shared_down, index * shared_width, shared_width, 0)
        act = (jax.nn.silu(jnp.dot(normed, s_gate, preferred_element_type=jnp.float32)) * jnp.dot(normed, s_up, preferred_element_type=jnp.float32)).astype(jnp.bfloat16)
        term = jnp.dot(act, s_down, preferred_element_type=jnp.float32)

        def one_expert(acc, pieces):
            gate_w, up_w, down_w, rows, weight = pieces
            taken = normed[rows]
            gate_blk = lax.dynamic_slice_in_dim(gate_w, index * expert_width, expert_width, 1)
            up_blk = lax.dynamic_slice_in_dim(up_w, index * expert_width, expert_width, 1)
            down_blk = lax.dynamic_slice_in_dim(down_w, index * expert_width, expert_width, 0)
            act_e = (jax.nn.silu(jnp.dot(taken, gate_blk, preferred_element_type=jnp.float32)) * jnp.dot(taken, up_blk, preferred_element_type=jnp.float32)).astype(jnp.bfloat16)
            part = round_trip(jnp.dot(act_e, down_blk, preferred_element_type=jnp.float32))
            return (acc.at[rows].add(part * weight[:, None]), None)
        term, _ = lax.scan(one_expert, term, (expert_gate, expert_up, expert_down, rows_of, weight_of))
        return (total + round_trip(term), None)
    moe, _ = lax.scan(width_block, jnp.zeros((TOKENS, D), jnp.float32), jnp.arange(N_TP, dtype=jnp.int32))
    return (hidden_state.astype(jnp.float32) + moe).astype(jnp.bfloat16)
```

```python
import functools

import jax
import jax.numpy as jnp
from jax import lax
from jax.experimental import pallas as pl
from jax.experimental.pallas import tpu as pltpu
from jax.sharding import PartitionSpec as P

DA = 64
VA = 64
DB = 128
VB = 128
ROPE = 32


theta_base = 10000.0
norm_eps = 1e-06
very_low = -1e30
kernel_vmem = 20 * 2**20

MESH_ID = pl.DeviceIdType.MESH
VMEM_SPEC = pl.BlockSpec(memory_space=pltpu.VMEM)


def remote(src, dst, send, recv, device):
    return pltpu.make_async_remote_copy(
        src_ref=src, dst_ref=dst, send_sem=send, recv_sem=recv, device_id=device,
        device_id_type=MESH_ID,
    )


def greet(devices):
    barrier = pltpu.get_barrier_semaphore()
    for device in devices:
        pl.semaphore_signal(barrier, inc=1, device_id=device, device_id_type=MESH_ID)
    pl.semaphore_wait(barrier, len(devices))


def place_in_tp():
    me = lax.axis_index("tp")
    core = lax.rem(me, 2)
    return me, core, me // 2, {"tp": me + 1 - 2 * core}


def block_of(chips, chip, core):
    return core * chips + chip


def all_peers(n, chips):
    me = lax.axis_index("sp")
    near, mate = tp_chip_peers(chips)
    return [{"sp": lax.rem(me + k, n)} for k in range(1, n)], near + [mate]


def spread(chips, count, arrive, slot, ysend, yrecv, msend, mrecv):
    _, core, chip, mate = place_in_tp()
    near, far = [], []

    def relay(item):
        for i, j, copy in far:
            if i == item:
                copy.wait_recv()
                block = slot(i, block_of(chips, lax.rem(chip + chips - j, chips), core))
                onward = remote(block, block, msend.at[j, i], mrecv.at[j, i], mate)
                onward.start()
                near.append(onward)

    for i in range(count):
        arrive(i)
        own = slot(i, block_of(chips, chip, core))
        for j in range(1, chips):
            copy = remote(
                own, own, ysend.at[j - 1, i], yrecv.at[j - 1, i],
                {"tp": 2 * lax.rem(chip + j, chips) + core},
            )
            copy.start()
            far.append((i, j, copy))
        copy = remote(own, own, msend.at[0, i], mrecv.at[0, i], mate)
        copy.start()
        near.append(copy)
        if i:
            relay(i - 1)
    relay(count - 1)
    for _, _, copy in far:
        copy.wait_send()
    for copy in near:
        copy.wait()


def spread_sems(chips, count):
    return [pltpu.SemaphoreType.DMA((chips - 1, count))] * 2 + [
        pltpu.SemaphoreType.DMA((chips, count))
    ] * 2


def gather_kernel(n, lat_ref, rot_ref, lat_out, rot_out, send, recv, fsend, frecv, local):
    me = lax.axis_index("sp")
    _, core, _, mate = place_in_tp()
    pairs = ((lat_ref, lat_out), (rot_ref, rot_out))
    own = [
        pltpu.make_async_copy(src, dst.at[me], local.at[a]) for a, (src, dst) in enumerate(pairs)
    ]
    for copy in own:
        copy.start()
    peers = [{"sp": lax.rem(me + k, n)} for k in range(1, n)]
    greet(peers + [mate])
    copies = []
    for k in range(1, n):
        for a, (src, dst) in enumerate(pairs):
            copy = remote(
                src.at[core], dst.at[me, core], send.at[a, k - 1], recv.at[a, k - 1], peers[k - 1]
            )
            copy.start()
            copies.append(copy)
    forwards = []
    for k in range(1, n):
        origin = lax.rem(me + n - k, n)
        for a, (src, dst) in enumerate(pairs):
            copies[2 * (k - 1) + a].wait_recv()
            forward = remote(
                dst.at[origin, core], dst.at[origin, core], fsend.at[a, k - 1],
                frecv.at[a, k - 1], mate,
            )
            forward.start()
            forwards.append(forward)
    for copy in own:
        copy.wait()
    for copy in copies:
        copy.wait_send()
    for forward in forwards:
        forward.wait()


def gather_latents(latents, rot_key):
    n = lax.axis_size("sp")
    tok, rank = latents.shape
    rope = rot_key.shape[1]
    half = tok // 2
    lat, rot = pl.pallas_call(
        functools.partial(gather_kernel, n),
        out_shape=(
            jax.ShapeDtypeStruct((n, 2, half, rank), latents.dtype),
            jax.ShapeDtypeStruct((n, 2, half * rope // 128, 128), rot_key.dtype),
        ),
        in_specs=[VMEM_SPEC] * 2,
        out_specs=(VMEM_SPEC,) * 2,
        scratch_shapes=[pltpu.SemaphoreType.DMA((2, n - 1))] * 4 + [pltpu.SemaphoreType.DMA((2,))],
        compiler_params=pltpu.CompilerParams(collective_id=0, has_side_effects=True, vmem_limit_bytes=kernel_vmem),
        name="gather_latents",
    )(latents.reshape(2, half, rank), rot_key.reshape(2, half * rope // 128, 128))
    return lat.reshape(n * tok, rank), rot.reshape(n * tok, rope)


def scatter_sum(chips, term_ref, base_ref, from_mate, pair, landed, sems):
    psend, precv, csend, crecv = sems
    me, core, chip, mate = place_in_tp()
    first = []
    for k in list(range(1, chips)) + [0]:
        where = lax.rem(chip + k, chips)
        copy = remote(
            term_ref.at[2 * where + 1 - core], from_mate.at[k], psend.at[k], precv.at[k], mate
        )
        copy.start()
        first.append((k, where, copy))
    second = []
    for k, where, copy in first:
        copy.wait_recv()
        total = term_ref[2 * where + core].astype(jnp.float32) + from_mate[k].astype(jnp.float32)
        if k:
            pair[k - 1] = total.astype(jnp.bfloat16)
            out = remote(
                pair.at[k - 1], landed.at[k - 1], csend.at[k - 1], crecv.at[k - 1],
                {"tp": 2 * where + core},
            )
            out.start()
            second.append(out)
    for k, out in enumerate(second):
        out.wait_recv()
        total = total + landed[k].astype(jnp.float32)
    for _, _, copy in first:
        copy.wait_send()
    for out in second:
        out.wait_send()
    return base_ref[...].astype(jnp.float32) + total


def tp_chip_peers(chips):
    _, core, chip, mate = place_in_tp()
    return [{"tp": 2 * lax.rem(chip + k, chips) + core} for k in range(1, chips)], mate


def norm_kernel(
    chips, term_ref, base_ref, gain_ref, hidden_ref, rows_ref,
    from_mate, pair, landed, psend, precv, csend, crecv, asend, arecv, fsend, frecv,
):
    me, core, chip, mate = place_in_tp()
    peers, _ = tp_chip_peers(chips)
    greet(peers + [mate])
    state = scatter_sum(
        chips, term_ref, base_ref, from_mate, pair, landed, (psend, precv, csend, crecv)
    ).astype(jnp.bfloat16)
    hidden_ref[...] = state
    wide = state.astype(jnp.float32)
    normed = wide * lax.rsqrt(jnp.mean(wide * wide, axis=-1, keepdims=True) + norm_eps)
    rows_ref[me] = (normed * gain_ref[...]).astype(jnp.bfloat16)
    copies = []
    for k in range(1, chips):
        copy = remote(rows_ref.at[me], rows_ref.at[me], asend.at[k], arecv.at[k], peers[k - 1])
        copy.start()
        copies.append(copy)
    near = remote(rows_ref.at[me], rows_ref.at[me], asend.at[0], arecv.at[0], mate)
    near.start()
    forwards = []
    for k in range(1, chips):
        copies[k - 1].wait_recv()
        origin = 2 * lax.rem(chip + chips - k, chips) + core
        forward = remote(
            rows_ref.at[origin], rows_ref.at[origin], fsend.at[k - 1], frecv.at[k - 1], mate
        )
        forward.start()
        forwards.append(forward)
    near.wait()
    for copy in copies:
        copy.wait_send()
    for forward in forwards:
        forward.wait()


def final_kernel(
    chips, term_ref, base_ref, out_ref, from_mate, pair, landed, psend, precv, csend, crecv
):
    peers, mate = tp_chip_peers(chips)
    greet(peers + [mate])
    out_ref[...] = scatter_sum(
        chips, term_ref, base_ref, from_mate, pair, landed, (psend, precv, csend, crecv)
    ).astype(jnp.bfloat16)


def sum_scratch(chips, rows, width):
    return [
        pltpu.VMEM((chips, rows, width), jnp.bfloat16),
        pltpu.VMEM((chips - 1, rows, width), jnp.bfloat16),
        pltpu.VMEM((chips - 1, rows, width), jnp.bfloat16),
        pltpu.SemaphoreType.DMA((chips,)),
        pltpu.SemaphoreType.DMA((chips,)),
        pltpu.SemaphoreType.DMA((chips - 1,)),
        pltpu.SemaphoreType.DMA((chips - 1,)),
    ]


def mix_and_norm(term, residual, gain):
    devices = lax.axis_size("tp")
    chips = devices // 2
    rows, width = residual.shape
    hidden, whole = pl.pallas_call(
        functools.partial(norm_kernel, chips),
        out_shape=(
            jax.ShapeDtypeStruct((rows, width), jnp.bfloat16),
            jax.ShapeDtypeStruct((devices, rows, width), jnp.bfloat16),
        ),
        in_specs=[VMEM_SPEC] * 3,
        out_specs=(VMEM_SPEC,) * 2,
        scratch_shapes=sum_scratch(chips, rows, width)
        + [pltpu.SemaphoreType.DMA((chips,))] * 2
        + [pltpu.SemaphoreType.DMA((chips - 1,))] * 2,
        compiler_params=pltpu.CompilerParams(collective_id=1, has_side_effects=True, vmem_limit_bytes=kernel_vmem),
        name="mix_and_norm",
    )(term.reshape(devices, rows, width), residual, gain.reshape(1, width))
    return hidden, whole.reshape(devices * rows, width)


def final_sum(term, hidden):
    devices = lax.axis_size("tp")
    chips = devices // 2
    rows, width = hidden.shape
    return pl.pallas_call(
        functools.partial(final_kernel, chips),
        out_shape=jax.ShapeDtypeStruct((rows, width), jnp.bfloat16),
        in_specs=[VMEM_SPEC] * 2,
        out_specs=VMEM_SPEC,
        scratch_shapes=sum_scratch(chips, rows, width),
        compiler_params=pltpu.CompilerParams(collective_id=4, has_side_effects=True, vmem_limit_bytes=kernel_vmem),
        name="final_sum",
    )(term.reshape(devices, rows, width), hidden)


def dispatch_kernel(n, chips, out_ref, got_ref, send, recv, local, *sems):
    me = lax.axis_index("sp")
    _, core, chip, _ = place_in_tp()
    mine = block_of(chips, chip, core)
    cols = out_ref.shape[2]

    def slot(source, block):
        return got_ref.at[source, :, pl.ds(pl.multiple_of(block * cols, cols), cols)]

    own = pltpu.make_async_copy(out_ref.at[me], slot(me, mine), local.at[0])
    own.start()
    peers, group = all_peers(n, chips)
    greet(peers + group)
    copies = []
    for k in range(1, n):
        copy = remote(
            out_ref.at[lax.rem(me + k, n)], slot(me, mine), send.at[k], recv.at[k], peers[k - 1]
        )
        copy.start()
        copies.append(copy)
    spread(
        chips,
        n,
        lambda i: copies[i - 1].wait_recv() if i else own.wait(),
        lambda i, block: slot(lax.rem(me + n - i, n), block),
        *sems,
    )
    for copy in copies:
        copy.wait_send()


def dispatch(outgoing):
    n, items, cols = outgoing.shape
    devices = lax.axis_size("tp")
    return pl.pallas_call(
        functools.partial(dispatch_kernel, n, devices // 2),
        out_shape=jax.ShapeDtypeStruct((n, items, cols * devices), jnp.bfloat16),
        in_specs=[VMEM_SPEC],
        out_specs=VMEM_SPEC,
        scratch_shapes=[pltpu.SemaphoreType.DMA((n,))] * 2
        + [pltpu.SemaphoreType.DMA((1,))]
        + spread_sems(devices // 2, n),
        compiler_params=pltpu.CompilerParams(collective_id=2, has_side_effects=True, vmem_limit_bytes=kernel_vmem),
        name="dispatch",
    )(outgoing)


def return_kernel(
    n, chips, part_ref, back_ref, from_mate, pair, landed, ready,
    psend, precv, ysend, yrecv, send, recv,
):
    me = lax.axis_index("sp")
    _, core, chip, mate = place_in_tp()
    cols = back_ref.shape[2]
    half = cols * chips
    peers, group = all_peers(n, chips)
    greet(peers + group)

    def columns(start, width):
        return pl.ds(pl.multiple_of(start * width, width), width)

    order = list(range(1, n)) + [0]
    first, second, third = [], [], []
    for k in order:
        copy = remote(
            part_ref.at[lax.rem(me + k, n), :, columns(1 - core, half)], from_mate.at[k],
            psend.at[k], precv.at[k], mate,
        )
        copy.start()
        first.append(copy)
    for k, copy in zip(order, first):
        copy.wait_recv()
        total = part_ref[lax.rem(me + k, n), :, columns(core, half)].astype(jnp.float32)
        pair[k] = (total + from_mate[k].astype(jnp.float32)).astype(jnp.bfloat16)
        for j in range(1, chips):
            where = lax.rem(chip + j, chips)
            out = remote(
                pair.at[k, :, columns(where, cols)], landed.at[j - 1, k],
                ysend.at[j - 1, k], yrecv.at[j - 1, k], {"tp": 2 * where + core},
            )
            out.start()
            second.append((k, j, out))
    for k in order:
        total = pair[k, :, columns(chip, cols)].astype(jnp.float32)
        for i, j, out in second:
            if i == k:
                out.wait_recv()
                total = total + landed[j - 1, k].astype(jnp.float32)
        if k:
            ready[k - 1] = total.astype(jnp.bfloat16)
            home = remote(
                ready.at[k - 1], back_ref.at[me], send.at[k - 1], recv.at[k - 1], peers[k - 1]
            )
            home.start()
            third.append(home)
        else:
            back_ref[me] = total.astype(jnp.bfloat16)
    for copy in first:
        copy.wait_send()
    for _, _, out in second:
        out.wait_send()
    for home in third:
        home.wait()


def return_parts(part):
    n, items, width = part.shape
    devices = lax.axis_size("tp")
    chips = devices // 2
    cols = width // devices
    return pl.pallas_call(
        functools.partial(return_kernel, n, chips),
        out_shape=jax.ShapeDtypeStruct((n, items, cols), jnp.bfloat16),
        in_specs=[VMEM_SPEC],
        out_specs=VMEM_SPEC,
        scratch_shapes=[
            pltpu.VMEM((n, items, width // 2), jnp.bfloat16),
            pltpu.VMEM((n, items, width // 2), jnp.bfloat16),
            pltpu.VMEM((chips - 1, n, items, cols), jnp.bfloat16),
            pltpu.VMEM((n - 1, items, cols), jnp.bfloat16),
            pltpu.SemaphoreType.DMA((n,)),
            pltpu.SemaphoreType.DMA((n,)),
            pltpu.SemaphoreType.DMA((chips - 1, n)),
            pltpu.SemaphoreType.DMA((chips - 1, n)),
            pltpu.SemaphoreType.DMA((n - 1,)),
            pltpu.SemaphoreType.DMA((n - 1,)),
        ],
        compiler_params=pltpu.CompilerParams(collective_id=3, has_side_effects=True, vmem_limit_bytes=kernel_vmem),
        name="return_parts",
    )(part)


def whole_block(shape):
    return pl.BlockSpec(shape, lambda i: (0,) * len(shape))


def column_block(shape, cols):
    return pl.BlockSpec((shape[0], cols), lambda i: (0, i))


def column_call(body, name, whole, tiled, rows, cols, dtype, flops):
    width = tiled[0].shape[1]
    moved = sum(a.size * a.dtype.itemsize for a in (*whole, *tiled)) + rows * width * 2
    return pl.pallas_call(
        body,
        out_shape=jax.ShapeDtypeStruct((rows, width), dtype),
        grid=(width // cols,),
        in_specs=[whole_block(a.shape) for a in whole]
        + [column_block(a.shape, cols) for a in tiled],
        out_specs=column_block((rows, width), cols),
        cost_estimate=pl.CostEstimate(flops=flops, bytes_accessed=moved, transcendentals=0),
        compiler_params=pltpu.CompilerParams(dimension_semantics=("arbitrary",), vmem_limit_bytes=kernel_vmem),
        name=name,
    )(*whole, *tiled)


def dot32(a, b):
    return jnp.dot(a, b, preferred_element_type=jnp.float32)


def tile_of(width, most):
    cols = min(width, most)
    return cols if width % cols == 0 else 128


def gated_body(rows_ref, gate_ref, up_ref, out_ref):
    gate = dot32(rows_ref[...], gate_ref[...])
    up = dot32(rows_ref[...], up_ref[...])
    out_ref[...] = (gate / (1.0 + jnp.exp(-gate)) * up).astype(jnp.bfloat16)


def gated(rows, gate, up, name):
    count, width = rows.shape
    hidden = gate.shape[1]
    return column_call(
        gated_body, name, (rows,), (gate, up), count, tile_of(hidden, 256), jnp.bfloat16,
        4 * count * width * hidden,
    )


def product_body(rows_ref, weight_ref, out_ref):
    out_ref[...] = dot32(rows_ref[...], weight_ref[...]).astype(jnp.bfloat16)


def product(rows, weight, name):
    return column_call(
        product_body, name, (rows,), (weight,), rows.shape[0], tile_of(weight.shape[1], 512),
        jnp.bfloat16, 2 * rows.shape[0] * weight.size,
    )


def project_body(a_ref, b_ref, pa_ref, pb_ref, out_ref):
    total = jnp.zeros(out_ref.shape, jnp.float32)
    for heads_ref, weight_ref in ((a_ref, pa_ref), (b_ref, pb_ref)):
        size = heads_ref.shape[2]
        for h in range(heads_ref.shape[0]):
            total += dot32(heads_ref[h], weight_ref[h * size : (h + 1) * size, :])
    out_ref[...] = total.astype(jnp.bfloat16)


def project(heads_a, heads_b, proj_a, proj_b):
    rows = heads_a.shape[1]
    return column_call(
        project_body, "project", (heads_a, heads_b), (proj_a, proj_b), rows,
        tile_of(proj_a.shape[1], 512), jnp.bfloat16, 2 * rows * (proj_a.size + proj_b.size),
    )


def combine_body(act_ref, back_ref, slots_ref, weights_ref, down_ref, out_ref):
    _, core, chip, _ = place_in_tp()
    block = block_of(lax.axis_size("tp") // 2, chip, core)
    term = dot32(act_ref[...], down_ref[...])
    here = pl.program_id(0) == block

    @pl.when(here)
    def _():
        total = term
        spots = lax.broadcasted_iota(jnp.int32, (act_ref.shape[0], back_ref.shape[0]), 1)
        for k in range(slots_ref.shape[1]):
            chosen = (spots == slots_ref[:, k : k + 1]).astype(jnp.float32).astype(jnp.bfloat16)
            total += dot32(chosen, back_ref[...]) * weights_ref[:, k : k + 1]
        out_ref[...] = total.astype(jnp.bfloat16)

    @pl.when(jnp.logical_not(here))
    def _():
        out_ref[...] = term.astype(jnp.bfloat16)


def tables(positions, width):
    half = width // 2
    freqs = theta_base ** (-(2.0 * jnp.arange(half, dtype=jnp.float32)) / width)
    angles = positions.astype(jnp.float32)[:, None] * freqs[None, :]
    return (jnp.cos(angles), jnp.sin(angles))


def rotate(values, cosine, sine):
    half = values.shape[-1] // 2
    first = values[..., :half].astype(jnp.float32)
    second = values[..., half:].astype(jnp.float32)
    turned = jnp.concatenate(
        [first * cosine - second * sine, first * sine + second * cosine], axis=-1
    )
    return turned.astype(jnp.bfloat16)


def group_update(state, queries_nope, queries_rope, keys, values, rot_piece, mask, scale):
    top, total, weighted = state
    scores = jnp.einsum("qhd,khd->hqk", queries_nope, keys, preferred_element_type=jnp.float32)
    scores = scores + jnp.einsum(
        "qhr,kr->hqk", queries_rope, rot_piece, preferred_element_type=jnp.float32
    )
    scores = jnp.where(mask[None], scores * scale, very_low)
    new_top = jnp.maximum(top, jnp.max(scores, axis=-1))
    expo = jnp.where(mask[None], jnp.exp(scores - new_top[..., None]), 0.0)
    total = jnp.sum(expo, axis=-1)
    weighted = jnp.einsum(
        "hqk,khv->hqv", expo.astype(jnp.bfloat16), values, preferred_element_type=jnp.float32
    )
    return (new_top, total, weighted)


def empty_state(heads, rows, vsize):
    return (
        jnp.full((heads, rows), very_low, jnp.float32),
        jnp.zeros((heads, rows), jnp.float32),
        jnp.zeros((heads, rows, vsize), jnp.float32),
    )


def shards(
    residual,
    query_a,
    query_b,
    latents,
    rope_key,
    key_up_a,
    value_up_a,
    key_up_b,
    value_up_b,
    out_proj_a,
    out_proj_b,
    norm_gain,
    routes,
    route_weights,
    shared_gate,
    shared_up,
    shared_down,
    expert_gate,
    expert_up,
    expert_down,
):
    tok = query_a.shape[0]
    heads_a = key_up_a.shape[1] // DA
    heads_b = key_up_b.shape[1] // DB
    first_row = lax.axis_index("sp") * tok
    query_pos = first_row + jnp.arange(tok, dtype=jnp.int32)
    cosine, sine = tables(query_pos, ROPE)
    rot_key = rotate(rope_key, cosine, sine)
    shaped_a = query_a.reshape(tok, heads_a, DA + ROPE)
    shaped_b = query_b.reshape(tok, heads_b, DB + ROPE)
    nope_a = shaped_a[..., :DA]
    nope_b = shaped_b[..., :DB]
    turned_a = rotate(shaped_a[..., DA:], cosine[:, None, :], sine[:, None, :])
    turned_b = rotate(shaped_b[..., DB:], cosine[:, None, :], sine[:, None, :])
    scale_a = (DA + ROPE) ** (-0.5)
    scale_b = (DB + ROPE) ** (-0.5)

    def attend(state, keys_a, values_a, keys_b, values_b, rot_piece, key_pos):
        count = keys_a.shape[0]
        mask = key_pos[None, :] <= query_pos[:, None]
        state_a = group_update(
            state[0],
            nope_a,
            turned_a,
            keys_a.reshape(count, heads_a, DA),
            values_a.reshape(count, heads_a, VA),
            rot_piece,
            mask,
            scale_a,
        )
        state_b = group_update(
            state[1],
            nope_b,
            turned_b,
            keys_b.reshape(count, heads_b, DB),
            values_b.reshape(count, heads_b, VB),
            rot_piece,
            mask,
            scale_b,
        )
        return (state_a, state_b)

    def project_latents(lat_rows):
        keys_a = jnp.dot(lat_rows, key_up_a, preferred_element_type=jnp.float32).astype(
            jnp.bfloat16
        )
        values_a = jnp.dot(lat_rows, value_up_a, preferred_element_type=jnp.float32).astype(
            jnp.bfloat16
        )
        keys_b = jnp.dot(lat_rows, key_up_b, preferred_element_type=jnp.float32).astype(
            jnp.bfloat16
        )
        values_b = jnp.dot(lat_rows, value_up_b, preferred_element_type=jnp.float32).astype(
            jnp.bfloat16
        )
        return (keys_a, values_a, keys_b, values_b)

    start_state = (empty_state(heads_a, tok, VA), empty_state(heads_b, tok, VB))
    lat_rows, rot_piece = gather_latents(latents, rot_key)
    key_pos = jnp.arange(lat_rows.shape[0], dtype=jnp.int32)

    def compute(inner):
        keys_a, values_a, keys_b, values_b = project_latents(lat_rows)
        return attend(inner, keys_a, values_a, keys_b, values_b, rot_piece, key_pos)

    state = compute(start_state)
    heads_out_a = (state[0][2] / state[0][1][..., None]).astype(jnp.bfloat16)
    heads_out_b = (state[1][2] / state[1][1][..., None]).astype(jnp.bfloat16)
    term = project(heads_out_a, heads_out_b, out_proj_a, out_proj_b)
    hidden_state, whole_rows = mix_and_norm(term, residual, norm_gain)
    shared_act = gated(whole_rows, shared_gate, shared_up, "shared_act")
    experts = lax.axis_size("sp")
    topk = routes.shape[1]
    capacity = max(2, 3 * tok * topk // (2 * experts))
    flat = routes.reshape(-1)
    onehot = (flat[:, None] == jnp.arange(experts, dtype=jnp.int32)[None, :]).astype(jnp.int32)
    before = jnp.cumsum(onehot, axis=0) - onehot
    rank = jnp.sum(before * onehot, axis=1)
    slots = (flat * capacity + rank).reshape(tok, topk)
    spots = jnp.arange(experts * capacity, dtype=jnp.int32)
    chosen = (slots[:, :, None] == spots[None, None, :]).astype(jnp.bfloat16)
    devices = lax.axis_size("tp")
    me = lax.axis_index("tp")
    width = whole_rows.shape[1]
    cols = width // devices
    start = block_of(devices // 2, me // 2, lax.rem(me, 2)) * cols
    outgoing = jnp.einsum(
        "rs,rd->sd",
        jnp.sum(chosen, axis=1),
        lax.dynamic_slice_in_dim(whole_rows, start, cols, axis=1),
        preferred_element_type=jnp.float32,
    ).astype(jnp.bfloat16)
    gate_w = expert_gate[0]
    up_w = expert_up[0]
    down_w = expert_down[0]
    arrived = dispatch(outgoing.reshape(experts, capacity, cols))
    rows_in = arrived.reshape(experts * capacity, width)
    act = gated(rows_in, gate_w, up_w, "expert_act")
    part = product(act, down_w, "expert_part")
    back = return_parts(part.reshape(experts, capacity, width))
    back_flat = back.reshape(experts * capacity, cols)
    term = column_call(
        combine_body, "combine", (shared_act, back_flat, slots, route_weights), (shared_down,), tok,
        cols, jnp.bfloat16, 2 * tok * shared_down.size,
    )
    return final_sum(term, hidden_state)


def solution(mesh):
    placed = (
        P(("sp", "tp"), None),
        P("sp", "tp"),
        P("sp", "tp"),
        P("sp", None),
        P("sp", None),
        P(None, "tp"),
        P(None, "tp"),
        P(None, "tp"),
        P(None, "tp"),
        P("tp", None),
        P("tp", None),
        P(),
        P("sp", None),
        P("sp", None),
        P(None, "tp"),
        P(None, "tp"),
        P("tp", None),
        P("sp", None, "tp"),
        P("sp", None, "tp"),
        P("sp", "tp", None),
    )
    return jax.shard_map(
        shards, mesh=mesh, in_specs=placed, out_specs=P(("sp", "tp"), None), check_vma=False
    )
```
